512 devices in a mesh: sp: 16 (over z), dp: 32 (over y, x, core).
Axes of the slice: x: 4, y: 4, z: 16, core: 2. Of those that a mesh axis runs over, the one named last changes fastest.
Arguments:
- queries: bfloat16 [32, 3072, 16, 128], P('dp', 'sp'), may hold values from -6 to 6
- keys: bfloat16 [32, 3072, 16, 128], P('dp', 'sp'), may hold values from -6 to 6
- values: bfloat16 [32, 3072, 16, 128], P('dp', 'sp'), may hold values from -6 to 6
- mix_ratio: float32 [16], replicated, may hold values from 0.3 to 0.8
- out_gain: float32 [128], replicated, may hold values from 0.1 to 1.9
- out_weight: bfloat16 [2048, 2048], P(None, 'dp'), may hold values from -0.125 to 0.125
Outputs:
- layer_out: bfloat16 [32, 3072, 2048], P('dp', 'sp')
The draws below stay inside these ranges and needn't reach their ends.
All inputs are finite; a program needn't handle non-finite values.
Results may differ from the reference program's by a relative error of at most 0.0098.
Values may be sent and summed in bfloat16 or wider, within the bound.
No kernel may reach another device: no remote copies, remote signals or barrier semaphores. Data moves between devices by JAX's collectives and lax.ppermute only.
A program may use at most 64 MiB of HBM per device.

```python
import math
import jax
import jax.numpy as jnp
from jax import lax

D = 2048
HEADS = 16
KEY_DIM = 64
HEAD_DIM = 128
SEQS = 32
LENGTH = 3072


def score_field(key, salt):
    shape = (SEQS, LENGTH, HEADS, 2 * KEY_DIM)
    spread = jnp.clip(1.3 * jax.random.normal(jax.random.fold_in(key, salt), shape, jnp.float32), -6.0, 6.0)
    return spread.astype(jnp.bfloat16)


def draw_queries(key, part):
    return score_field(key, 1)


def draw_keys(key, part):
    return score_field(key, 2)


def block_levels(stream_key, dims, shards, smallest, high):
    level, own = 1.0, jax.random.fold_in(stream_key, 6)
    for dim, blocks in shards:
        heights = jnp.exp(jax.random.uniform(jax.random.fold_in(own, dim), (blocks,), jnp.float32, smallest / len(shards), high / len(shards)))
        level = level * jnp.repeat(heights, dims[dim] // blocks).reshape([-1 if axis == dim else 1 for axis in range(len(dims))])
    return level


def bell_draw(rng, shape, scale, bound, pieces=(), kind=jnp.bfloat16):
    loudness = block_levels(rng, shape, pieces, -0.22, 0.18) if pieces else 1.0
    array = jax.random.normal(rng, shape, jnp.float32) * scale * loudness
    return jnp.minimum(jnp.maximum(array, -bound), bound).astype(kind)


def setup_inputs(seed: int = 0) -> dict:
    streams_of = jax.random.split(jax.random.key(seed), 7)
    return {
        "queries": draw_queries(jax.random.fold_in(streams_of[6], 71), 0),
        "keys": draw_keys(jax.random.fold_in(streams_of[6], 71), 0),
        "values": bell_draw(streams_of[2], (SEQS, LENGTH, HEADS, HEAD_DIM), 1.0, 6.0, ((0, 32), (1, 16))),
        "mix_ratio": jnp.clip(jax.random.uniform(streams_of[3], (HEADS,), jnp.float32, 0.3, 0.8), 0.3, 0.8),
        "out_gain": jnp.clip(1.0 + 0.18 * jax.random.normal(streams_of[4], (HEAD_DIM,), jnp.float32), 0.1, 1.9),
        "out_weight": bell_draw(streams_of[5], (HEADS * HEAD_DIM, D), (HEADS * HEAD_DIM) ** -0.5, 0.125, ((1, 32),)),
    }


theta_base = 500000.0
neg_large = -1e+30
norm_eps = 1e-05

def rotate_halves(field, positions):
    width = field.shape[-1] // 2
    half = width // 2
    freqs = theta_base ** (-jnp.arange(half, dtype=jnp.float32) * 2.0 / width)
    angle = positions.astype(jnp.float32)[:, None] * freqs[None, :]
    cosine = jnp.cos(angle)[:, None, :]
    sine = jnp.sin(angle)[:, None, :]
    parts = field.reshape(field.shape[0], 2, width)
    lower = parts[..., :half]
    upper = parts[..., half:]
    turned = jnp.concatenate([lower * cosine - upper * sine, upper * cosine + lower * sine], axis=-1)
    return turned.reshape(field.shape)

def masked_softmax(scores, visible):
    kept = jnp.where(visible, scores, neg_large)
    highest = lax.optimization_barrier(jnp.max(kept, axis=-1, keepdims=True))
    powers = jnp.exp(kept - highest)
    return powers / lax.optimization_barrier(jnp.sum(powers, axis=-1, keepdims=True))

def head_attention(query_head, key_head, value_head, ratio, gain):
    length = query_head.shape[0]
    width = query_head.shape[1] // 2
    positions = jnp.arange(length, dtype=jnp.int32)
    rotated_queries = (rotate_halves(query_head.astype(jnp.float32), positions) * width ** (-0.5)).astype(jnp.bfloat16)
    rotated_keys = rotate_halves(key_head.astype(jnp.float32), positions).astype(jnp.bfloat16)
    block = math.gcd(512, length)

    def one_block(start):
        query_rows = lax.dynamic_slice_in_dim(rotated_queries, start, block, 0)
        visible = (start + jnp.arange(block, dtype=jnp.int32))[:, None] >= positions[None, :]
        first = jnp.dot(query_rows[:, :width], rotated_keys[:, :width].T, preferred_element_type=jnp.float32)
        second = jnp.dot(query_rows[:, width:], rotated_keys[:, width:].T, preferred_element_type=jnp.float32)
        weights = (masked_softmax(first, visible) - ratio * masked_softmax(second, visible)).astype(jnp.bfloat16)
        mixed = jnp.dot(weights, value_head, preferred_element_type=jnp.float32)
        scale = lax.rsqrt(lax.optimization_barrier(jnp.mean(mixed * mixed, axis=-1, keepdims=True)) + norm_eps)
        return (mixed * scale * gain).astype(jnp.bfloat16)
    starts = jnp.arange(length // block, dtype=jnp.int32) * block
    return lax.map(one_block, starts).reshape(length, value_head.shape[1])

def reference(queries, keys, values, mix_ratio, out_gain, out_weight):

    def one_sequence(items):
        query_seq, key_seq, value_seq = items

        def one_head(head_items):
            query_head, key_head, value_head, ratio = head_items
            return head_attention(query_head, key_head, value_head, ratio, out_gain)
        heads = lax.map(one_head, (jnp.swapaxes(query_seq, 0, 1), jnp.swapaxes(key_seq, 0, 1), jnp.swapaxes(value_seq, 0, 1), mix_ratio))
        attended = jnp.swapaxes(heads, 0, 1).reshape(query_seq.shape[0], -1)
        return jnp.dot(attended, out_weight, preferred_element_type=jnp.float32).astype(jnp.bfloat16)
    return lax.map(one_sequence, (queries, keys, values))
```

```python
import functools

import jax
import jax.numpy as jnp
import numpy as np
from jax import lax
from jax.experimental import pallas as pl
from jax.experimental.pallas import tpu as pltpu
from jax.sharding import PartitionSpec as P

theta_base = 500000.0
neg_large = -1e30
norm_eps = 1e-05
TILE = 256


def turn_kernel(base_ref, freq_ref, q_ref, k_ref, out_ref):
    tokens, heads, width = q_ref.shape
    lane = lax.broadcasted_iota(jnp.int32, (tokens, width), 1)
    row = lax.broadcasted_iota(jnp.int32, (tokens, width), 0)
    first = base_ref[0] + pl.program_id(0) * tokens
    angle = (first + row).astype(jnp.float32) * freq_ref[...]
    lower = lane % 64 < 32
    cosine = jnp.cos(angle)[:, None, :]
    sine = jnp.where(lower, -jnp.sin(angle), jnp.sin(angle))[:, None, :]
    lower = jnp.broadcast_to(lower[:, None, :], (tokens, heads, width))

    def turned(x):
        flat = x.reshape(tokens * heads, width)
        up = pltpu.roll(flat, width - 32, 1).reshape(tokens, heads, width)
        down = pltpu.roll(flat, 32, 1).reshape(tokens, heads, width)
        return x * cosine + jnp.where(lower, up, down) * sine

    q = turned(q_ref[...].astype(jnp.float32)) * 0.125
    out_ref[:, 0] = jnp.swapaxes(q, 0, 1).astype(jnp.bfloat16)
    k = turned(k_ref[...].astype(jnp.float32))
    out_ref[:, 1] = jnp.swapaxes(k, 0, 1).astype(jnp.bfloat16)


def turn_and_group(q, k, first_position):
    tokens, heads, width = q.shape
    step = 48
    lanes = np.arange(width) % 32
    freqs = jnp.asarray((theta_base ** (-lanes * 2.0 / 64.0)).astype(np.float32)[None, :])
    block = pl.BlockSpec((step, heads, width), lambda i: (i, 0, 0))
    return pl.pallas_call(
        turn_kernel,
        name="turn",
        grid=(tokens // step,),
        in_specs=[
            pl.BlockSpec(memory_space=pltpu.SMEM),
            pl.BlockSpec((1, width), lambda i: (0, 0)),
            block,
            block,
        ],
        out_specs=pl.BlockSpec((heads, 2, step, width), lambda i: (0, 0, i, 0)),
        out_shape=jax.ShapeDtypeStruct((heads, 2, tokens, width), jnp.bfloat16),
    )(first_position, freqs, q, k)


def weights_kernel(ratio_ref, qk_ref, out_ref, q_s, k_s, s_s, m_s, l_s):
    planes, _, tokens, width = qk_ref.shape
    blocks = planes * tokens // TILE
    step = pl.program_id(0)

    @pl.when(step == 0)
    def _():
        for z in range(planes):
            q_s[z * tokens : (z + 1) * tokens, :] = qk_ref[z, 0]
            k_s[z * tokens : (z + 1) * tokens, :] = qk_ref[z, 1]

    ratio = ratio_ref[0]

    def one_row(row, at):
        q = q_s[pl.ds(pl.multiple_of(row * TILE, TILE), TILE), :]
        lane = lax.broadcasted_iota(jnp.int32, (TILE, width), 1)
        zero = jnp.zeros_like(q)
        both = jnp.concatenate([jnp.where(lane < 64, q, zero), jnp.where(lane < 64, zero, q)], axis=0)

        def tile_scores(j):
            keys = k_s[pl.ds(pl.multiple_of(j * TILE, TILE), TILE), :]
            return lax.dot_general(
                both, keys, (((1,), (1,)), ((), ())), preferred_element_type=jnp.float32
            )

        r = lax.broadcasted_iota(jnp.int32, (2 * TILE, TILE), 0)
        c = lax.broadcasted_iota(jnp.int32, (2 * TILE, TILE), 1)
        s = jnp.where(r % TILE >= c, tile_scores(row), neg_large)
        s_s[row] = s
        m_s[...] = jnp.maximum(s[:, :128], s[:, 128:])

        @pl.loop(0, row)
        def _(j):
            s = tile_scores(j)
            s_s[j] = s
            m_s[...] = jnp.maximum(m_s[...], jnp.maximum(s[:, :128], s[:, 128:]))

        top = jnp.max(m_s[...], axis=-1, keepdims=True)
        m_s[...] = jnp.broadcast_to(top, m_s.shape)
        l_s[...] = jnp.zeros_like(l_s)

        @pl.loop(0, row + 1)
        def _(j):
            s = s_s[j]
            m = m_s[...]
            e0 = jnp.exp(s[:, :128] - m)
            e1 = jnp.exp(s[:, 128:] - m)
            l_s[...] += e0 + e1
            s_s[j] = jnp.concatenate([e0, e1], axis=1)

        total = jnp.sum(l_s[...], axis=-1, keepdims=True)
        a1 = 1.0 / total[:TILE]
        a2 = ratio / total[TILE:]
        l_s[...] = jnp.broadcast_to(jnp.concatenate([a1, a2], axis=0), l_s.shape)

        @pl.loop(0, row + 1)
        def _(j):
            b1 = l_s[:TILE, :]
            b2 = l_s[TILE:, :]
            e = s_s[j]
            w0 = e[:TILE, :128] * b1 - e[TILE:, :128] * b2
            w1 = e[:TILE, 128:] * b1 - e[TILE:, 128:] * b2
            out_ref[0, at + j] = jnp.concatenate([w0, w1], axis=1).astype(jnp.bfloat16)

    one_row(step, 0)
    one_row(blocks - 1 - step, step + 1)


def attention_weights(ratio, qk):
    planes, _, tokens, width = qk.shape
    blocks = planes * tokens // TILE
    return pl.pallas_call(
        weights_kernel,
        name="weights",
        grid=(blocks // 2,),
        in_specs=[
            pl.BlockSpec(memory_space=pltpu.SMEM),
            pl.BlockSpec(qk.shape, lambda p: (0, 0, 0, 0)),
        ],
        out_specs=pl.BlockSpec((1, blocks + 1, TILE, TILE), lambda p: (p, 0, 0, 0)),
        out_shape=jax.ShapeDtypeStruct((blocks // 2, blocks + 1, TILE, TILE), jnp.bfloat16),
        scratch_shapes=[
            pltpu.VMEM((planes * tokens, width), jnp.bfloat16),
            pltpu.VMEM((planes * tokens, width), jnp.bfloat16),
            pltpu.VMEM((blocks, 2 * TILE, TILE), jnp.float32),
            pltpu.VMEM((2 * TILE, 128), jnp.float32),
            pltpu.VMEM((2 * TILE, 128), jnp.float32),
        ],
        cost_estimate=pl.CostEstimate(
            flops=8 * 10**9, bytes_accessed=14 * 10**6, transcendentals=10**7
        ),
    )(ratio, qk)


def mix_kernel(gain_ref, w_ref, v_ref, out_ref, v_s, o_s):
    planes, tokens, width = v_ref.shape
    blocks = planes * tokens // TILE
    step = pl.program_id(0)

    @pl.when(step == 0)
    def _():
        for z in range(planes):
            v_s[z * tokens : (z + 1) * tokens, :] = v_ref[z]

    def one_row(row, at):
        def add(j, acc):
            vals = v_s[pl.ds(pl.multiple_of(j * TILE, TILE), TILE), :]
            return acc + jnp.dot(w_ref[0, at + j], vals, preferred_element_type=jnp.float32)

        mixed = lax.fori_loop(0, row + 1, add, jnp.zeros((TILE, width), jnp.float32))
        scale = lax.rsqrt(jnp.mean(mixed * mixed, axis=-1, keepdims=True) + norm_eps)
        o_s[pl.ds(pl.multiple_of(row * TILE, TILE), TILE), :] = (
            mixed * scale * gain_ref[...]
        ).astype(jnp.bfloat16)

    one_row(step, 0)
    one_row(blocks - 1 - step, step + 1)

    @pl.when(step == blocks // 2 - 1)
    def _():
        for z in range(planes):
            out_ref[z] = o_s[z * tokens : (z + 1) * tokens, :]


def mix_values(gain, w, v):
    planes, tokens, width = v.shape
    blocks = planes * tokens // TILE
    whole = pl.BlockSpec(v.shape, lambda p: (0, 0, 0))
    return pl.pallas_call(
        mix_kernel,
        name="mix",
        grid=(blocks // 2,),
        in_specs=[
            pl.BlockSpec((1, width), lambda p: (0, 0)),
            pl.BlockSpec((1, blocks + 1, TILE, TILE), lambda p: (p, 0, 0, 0)),
            whole,
        ],
        out_specs=whole,
        out_shape=jax.ShapeDtypeStruct(v.shape, jnp.bfloat16),
        scratch_shapes=[
            pltpu.VMEM((planes * tokens, width), jnp.bfloat16),
            pltpu.VMEM((planes * tokens, width), jnp.bfloat16),
        ],
    )(gain, w, v)


def project_kernel(a_ref, w_ref, out_ref, a_s):
    heads, tokens, width = a_ref.shape

    @pl.when(pl.program_id(0) == 0)
    def _():
        for h in range(heads):
            a_s[:, h * width : (h + 1) * width] = a_ref[h]

    out_ref[...] = lax.dot_general(
        a_s[...], w_ref[...], (((1,), (1,)), ((), ())), preferred_element_type=jnp.float32
    ).astype(jnp.bfloat16)


def project(attended, weight_rows):
    heads, tokens, width = attended.shape
    columns = weight_rows.shape[0]
    step = 256
    return pl.pallas_call(
        project_kernel,
        name="project",
        grid=(columns // step,),
        in_specs=[
            pl.BlockSpec(attended.shape, lambda c: (0, 0, 0)),
            pl.BlockSpec((step, heads * width), lambda c: (c, 0)),
        ],
        out_specs=pl.BlockSpec((tokens, step), lambda c: (0, c)),
        out_shape=jax.ShapeDtypeStruct((tokens, columns), jnp.bfloat16),
        scratch_shapes=[pltpu.VMEM((tokens, heads * width), jnp.bfloat16)],
    )(attended, weight_rows)


def exchange(array):
    return lax.all_to_all(array, "sp", split_axis=0, concat_axis=0, tiled=True)


def on_device(queries, keys, values, mix_ratio, out_gain, out_weight):
    place = lax.axis_index("sp")
    tokens = queries.shape[1]
    first_position = (place * tokens).astype(jnp.int32).reshape(1)
    ratio = lax.dynamic_slice_in_dim(mix_ratio, place, 1, 0)
    weight_rows = lax.all_gather(out_weight.T, "dp", axis=0, tiled=True)
    qk = exchange(turn_and_group(queries[0], keys[0], first_position))
    by_head = jnp.swapaxes(values[0], 0, 1)
    by_head, qk = lax.optimization_barrier((by_head, qk))
    v = exchange(by_head)
    w = attention_weights(ratio, qk)
    attended = exchange(mix_values(out_gain[None, :], w, v))
    return project(attended, weight_rows)[None]


def solution(mesh):
    tokens = P("dp", "sp", None, None)
    return jax.shard_map(
        on_device,
        mesh=mesh,
        in_specs=(tokens, tokens, tokens, P(), P(), P(None, "dp")),
        out_specs=P("dp", "sp", None),
        check_vma=False,
    )
```

```python
import functools

import jax
import jax.numpy as jnp
import numpy as np
from jax import lax
from jax.experimental import pallas as pl
from jax.experimental.pallas import tpu as pltpu
from jax.sharding import PartitionSpec as P

theta_base = 500000.0
neg_large = -1e30
norm_eps = 1e-05
TILE = 256


def turn_kernel(base_ref, freq_ref, q_ref, k_ref, out_ref):
    tokens, heads, width = q_ref.shape
    lane = lax.broadcasted_iota(jnp.int32, (tokens, width), 1)
    row = lax.broadcasted_iota(jnp.int32, (tokens, width), 0)
    first = base_ref[0] + pl.program_id(0) * tokens
    angle = (first + row).astype(jnp.float32) * freq_ref[...]
    lower = lane % 64 < 32
    cosine = jnp.cos(angle)[:, None, :]
    sine = jnp.where(lower, -jnp.sin(angle), jnp.sin(angle))[:, None, :]
    lower = jnp.broadcast_to(lower[:, None, :], (tokens, heads, width))

    def turned(x):
        flat = x.reshape(tokens * heads, width)
        up = pltpu.roll(flat, width - 32, 1).reshape(tokens, heads, width)
        down = pltpu.roll(flat, 32, 1).reshape(tokens, heads, width)
        return x * cosine + jnp.where(lower, up, down) * sine

    q = turned(q_ref[...].astype(jnp.float32)) * 0.125
    out_ref[:, 0] = jnp.swapaxes(q, 0, 1).astype(jnp.bfloat16)
    k = turned(k_ref[...].astype(jnp.float32))
    out_ref[:, 1] = jnp.swapaxes(k, 0, 1).astype(jnp.bfloat16)


def turn_and_group(q, k, first_position):
    tokens, heads, width = q.shape
    step = 48
    lanes = np.arange(width) % 32
    freqs = jnp.asarray((theta_base ** (-lanes * 2.0 / 64.0)).astype(np.float32)[None, :])
    block = pl.BlockSpec((step, heads, width), lambda i: (i, 0, 0))
    return pl.pallas_call(
        turn_kernel,
        name="turn",
        grid=(tokens // step,),
        in_specs=[
            pl.BlockSpec(memory_space=pltpu.SMEM),
            pl.BlockSpec((1, width), lambda i: (0, 0)),
            block,
            block,
        ],
        out_specs=pl.BlockSpec((heads, 2, step, width), lambda i: (0, 0, i, 0)),
        out_shape=jax.ShapeDtypeStruct((heads, 2, tokens, width), jnp.bfloat16),
    )(first_position, freqs, q, k)


def weights_kernel(ratio_ref, qk_ref, out_ref, q_s, k_s, s_s, m_s, l_s):
    planes, _, tokens, width = qk_ref.shape
    blocks = planes * tokens // TILE
    step = pl.program_id(0)

    @pl.when(step == 0)
    def _():
        for z in range(planes):
            q_s[z * tokens : (z + 1) * tokens, :] = qk_ref[z, 0]
            k_s[z * tokens : (z + 1) * tokens, :] = qk_ref[z, 1]

    ratio = ratio_ref[0]

    def one_row(row, at):
        q = q_s[pl.ds(pl.multiple_of(row * TILE, TILE), TILE), :]
        lane = lax.broadcasted_iota(jnp.int32, (TILE, width), 1)
        zero = jnp.zeros_like(q)
        both = jnp.concatenate([jnp.where(lane < 64, q, zero), jnp.where(lane < 64, zero, q)], axis=0)

        def tile_scores(j):
            keys = k_s[pl.ds(pl.multiple_of(j * TILE, TILE), TILE), :]
            return lax.dot_general(
                both, keys, (((1,), (1,)), ((), ())), preferred_element_type=jnp.float32
            )

        r = lax.broadcasted_iota(jnp.int32, (2 * TILE, TILE), 0)
        c = lax.broadcasted_iota(jnp.int32, (2 * TILE, TILE), 1)
        s = jnp.where(r % TILE >= c, tile_scores(row), neg_large)
        s_s[row] = s
        m_s[...] = jnp.maximum(s[:, :128], s[:, 128:])

        @pl.loop(0, row)
        def _(j):
            s = tile_scores(j)
            s_s[j] = s
            m_s[...] = jnp.maximum(m_s[...], jnp.maximum(s[:, :128], s[:, 128:]))

        top = jnp.max(m_s[...], axis=-1, keepdims=True)
        m_s[...] = jnp.broadcast_to(top, m_s.shape)
        l_s[...] = jnp.zeros_like(l_s)

        @pl.loop(0, row + 1)
        def _(j):
            s = s_s[j]
            m = m_s[...]
            e0 = jnp.exp(s[:, :128] - m)
            e1 = jnp.exp(s[:, 128:] - m)
            l_s[...] += e0 + e1
            s_s[j] = jnp.concatenate([e0, e1], axis=1)

        total = jnp.sum(l_s[...], axis=-1, keepdims=True)
        a1 = 1.0 / total[:TILE]
        a2 = ratio / total[TILE:]
        l_s[...] = jnp.broadcast_to(jnp.concatenate([a1, a2], axis=0), l_s.shape)

        @pl.loop(0, row + 1)
        def _(j):
            b1 = l_s[:TILE, :]
            b2 = l_s[TILE:, :]
            e = s_s[j]
            w0 = e[:TILE, :128] * b1 - e[TILE:, :128] * b2
            w1 = e[:TILE, 128:] * b1 - e[TILE:, 128:] * b2
            lanes = pl.ds(pl.multiple_of((at + j) * TILE, TILE), TILE)
            out_ref[0, :, lanes] = jnp.concatenate([w0, w1], axis=1).astype(jnp.bfloat16)

    one_row(step, 0)
    one_row(blocks - 1 - step, step + 1)


def attention_weights(ratio, qk):
    planes, _, tokens, width = qk.shape
    blocks = planes * tokens // TILE
    return pl.pallas_call(
        weights_kernel,
        name="weights",
        grid=(blocks // 2,),
        in_specs=[
            pl.BlockSpec(memory_space=pltpu.SMEM),
            pl.BlockSpec(qk.shape, lambda p: (0, 0, 0, 0)),
        ],
        out_specs=pl.BlockSpec((1, TILE, (blocks + 1) * TILE), lambda p: (p, 0, 0)),
        out_shape=jax.ShapeDtypeStruct((blocks // 2, TILE, (blocks + 1) * TILE), jnp.bfloat16),
        scratch_shapes=[
            pltpu.VMEM((planes * tokens, width), jnp.bfloat16),
            pltpu.VMEM((planes * tokens, width), jnp.bfloat16),
            pltpu.VMEM((blocks, 2 * TILE, TILE), jnp.float32),
            pltpu.VMEM((2 * TILE, 128), jnp.float32),
            pltpu.VMEM((2 * TILE, 128), jnp.float32),
        ],
        cost_estimate=pl.CostEstimate(
            flops=8 * 10**9, bytes_accessed=14 * 10**6, transcendentals=10**7
        ),
    )(ratio, qk)


def mix_kernel(gain_ref, w_ref, v_ref, out_ref, w_s, sems):
    pairs = w_ref.shape[0]

    def fetch(p):
        return pltpu.make_async_copy(w_ref.at[p], w_s.at[p], sems.at[p])

    for p in range(pairs):
        fetch(p).start()
    for p in range(pairs):
        fetch(p).wait()
        split = (p + 1) * TILE
        for row, weights in ((p, w_s[p, :, :split]), (2 * pairs - 1 - p, w_s[p, :, split:])):
            mixed = jnp.dot(
                weights, v_ref[: (row + 1) * TILE, :], preferred_element_type=jnp.float32
            )
            scale = lax.rsqrt(jnp.mean(mixed * mixed, axis=-1, keepdims=True) + norm_eps)
            out_ref[row * TILE : (row + 1) * TILE, :] = (mixed * scale * gain_ref[...]).astype(
                jnp.bfloat16
            )


def mix_values(gain, w, v):
    planes, tokens, width = v.shape
    length = planes * tokens
    mixed = pl.pallas_call(
        mix_kernel,
        name="mix",
        in_specs=[
            pl.BlockSpec(memory_space=pltpu.VMEM),
            pl.BlockSpec(memory_space=pl.ANY),
            pl.BlockSpec(memory_space=pltpu.VMEM),
        ],
        out_specs=pl.BlockSpec(memory_space=pltpu.VMEM),
        out_shape=jax.ShapeDtypeStruct((length, width), jnp.bfloat16),
        scratch_shapes=[
            pltpu.VMEM(w.shape, jnp.bfloat16),
            pltpu.SemaphoreType.DMA((w.shape[0],)),
        ],
    )(gain, w, v.reshape(length, width))
    return mixed.reshape(planes, tokens, width)


def project_kernel(place_ref, a_ref, *refs):
    pieces, (out_ref, a_s, w_s, sems) = refs[:8], refs[8:]
    heads, tokens, width = a_ref.shape
    place = place_ref[0]
    y, x, core = place // 8, place // 2 % 4, place % 2
    rows = pieces[0].shape[1]

    def fetch(s, t, other):
        at = ((x + 4 - t) % 4) * 2 + (1 - core if other else core)
        return pltpu.make_async_copy(
            pieces[2 * s + other].at[t],
            w_s.at[s, pl.ds(pl.multiple_of(at * rows, rows), rows), :],
            sems.at[s, t, other],
        )

    every = [(t, other) for t in range(4) for other in range(2)]
    for s in range(4):
        for t, other in every:
            fetch(s, t, other).start()
    for h in range(heads):
        a_s[:, h * width : (h + 1) * width] = a_ref[h]
    for s in range(4):
        for t, other in every:
            fetch(s, t, other).wait()
        lanes = pl.ds(pl.multiple_of(((y + 4 - s) % 4) * 8 * rows, 8 * rows), 8 * rows)
        out_ref[:, lanes] = lax.dot_general(
            a_s[...], w_s[s], (((1,), (1,)), ((), ())), preferred_element_type=jnp.float32
        ).astype(jnp.bfloat16)


def project(place, attended, pieces):
    heads, tokens, width = attended.shape
    columns = 32 * pieces[0].shape[1]
    return pl.pallas_call(
        project_kernel,
        name="project",
        in_specs=[pl.BlockSpec(memory_space=pltpu.SMEM), pl.BlockSpec(memory_space=pltpu.VMEM)]
        + [pl.BlockSpec(memory_space=pl.ANY)] * len(pieces),
        out_specs=pl.BlockSpec(memory_space=pltpu.VMEM),
        out_shape=jax.ShapeDtypeStruct((tokens, columns), jnp.bfloat16),
        scratch_shapes=[
            pltpu.VMEM((tokens, heads * width), jnp.bfloat16),
            pltpu.VMEM((4, columns // 4, heads * width), jnp.bfloat16),
            pltpu.SemaphoreType.DMA((4, 4, 2)),
        ],
    )(place, attended, *pieces)


def shifted(array, dy, dx, flip):
    def to(i):
        y, x, core = i // 8, i // 2 % 4, i % 2
        return (y + dy) % 4 * 8 + (x + dx) % 4 * 2 + (1 - core if flip else core)

    return lax.ppermute(array, "dp", [(i, to(i)) for i in range(32)])


def gather_same_core(rows):
    line = jnp.stack([rows] + [shifted(rows, 0, d, False) for d in (1, 2, 3)])
    return [line] + [shifted(line, d, 0, False) for d in (1, 2, 3)]


def with_other_core(planes):
    pieces = []
    for plane in planes:
        pieces += [plane, shifted(plane, 0, 0, True)]
    return pieces


def exchange(array):
    return lax.all_to_all(array, "sp", split_axis=0, concat_axis=0, tiled=True)


def on_device(queries, keys, values, mix_ratio, out_gain, out_weight):
    plane = lax.axis_index("sp")
    place = lax.axis_index("dp").astype(jnp.int32).reshape(1)
    tokens = queries.shape[1]
    first_position = (plane * tokens).astype(jnp.int32).reshape(1)
    ratio = lax.dynamic_slice_in_dim(mix_ratio, plane, 1, 0)
    grouped = turn_and_group(queries[0], keys[0], first_position)
    grouped, rows = lax.optimization_barrier((grouped, out_weight.T))
    qk = exchange(grouped)
    planes = gather_same_core(rows)
    by_head = jnp.swapaxes(values[0], 0, 1)
    by_head, qk, planes = lax.optimization_barrier((by_head, qk, planes))
    v = exchange(by_head)
    w = attention_weights(ratio, qk)
    attended = exchange(mix_values(out_gain[None, :], w, v))
    return project(place, attended, with_other_core(planes))[None]


def solution(mesh):
    tokens = P("dp", "sp", None, None)
    return jax.shard_map(
        on_device,
        mesh=mesh,
        in_specs=(tokens, tokens, tokens, P(), P(), P(None, "dp")),
        out_specs=P("dp", "sp", None),
        check_vma=False,
    )
```

```python
import functools

import jax
import jax.numpy as jnp
import numpy as np
from jax import lax
from jax.experimental import pallas as pl
from jax.experimental.pallas import tpu as pltpu
from jax.sharding import PartitionSpec as P

theta_base = 500000.0
neg_large = -1e30
norm_eps = 1e-05
TILE = 256


def in_vmem(array):
    return pltpu.with_memory_space_constraint(array, pltpu.VMEM)


def limit(mebibytes):
    return pltpu.CompilerParams(vmem_limit_bytes=mebibytes * 2**20)


WHOLE = pl.BlockSpec(memory_space=pltpu.VMEM)
IN_HBM = pl.BlockSpec(memory_space=pltpu.HBM)
SCALARS = pl.BlockSpec(memory_space=pltpu.SMEM)


def turn_kernel(base_ref, freq_ref, q_ref, k_ref, out_ref):
    tokens, heads, width = q_ref.shape
    lane = lax.broadcasted_iota(jnp.int32, (tokens, width), 1)
    row = lax.broadcasted_iota(jnp.int32, (tokens, width), 0)
    first = base_ref[0] + pl.program_id(0) * tokens
    angle = (first + row).astype(jnp.float32) * freq_ref[...]
    lower = lane % 64 < 32
    cosine = jnp.cos(angle)[:, None, :]
    sine = jnp.where(lower, -jnp.sin(angle), jnp.sin(angle))[:, None, :]
    lower = jnp.broadcast_to(lower[:, None, :], (tokens, heads, width))

    def turned(x):
        flat = x.reshape(tokens * heads, width)
        up = pltpu.roll(flat, width - 32, 1).reshape(tokens, heads, width)
        down = pltpu.roll(flat, 32, 1).reshape(tokens, heads, width)
        return x * cosine + jnp.where(lower, up, down) * sine

    q = turned(q_ref[...].astype(jnp.float32)) * 0.125
    out_ref[:, 0] = jnp.swapaxes(q, 0, 1).astype(jnp.bfloat16)
    k = turned(k_ref[...].astype(jnp.float32))
    out_ref[:, 1] = jnp.swapaxes(k, 0, 1).astype(jnp.bfloat16)


def turn_and_group(q, k, first_position):
    tokens, heads, width = q.shape
    step = 48
    lanes = np.arange(width) % 32
    freqs = jnp.asarray((theta_base ** (-lanes * 2.0 / 64.0)).astype(np.float32)[None, :])
    block = pl.BlockSpec((step, heads, width), lambda i: (i, 0, 0))
    return pl.pallas_call(
        turn_kernel,
        name="turn",
        grid=(tokens // step,),
        in_specs=[
            pl.BlockSpec(memory_space=pltpu.SMEM),
            pl.BlockSpec((1, width), lambda i: (0, 0)),
            block,
            block,
        ],
        out_specs=pl.BlockSpec((heads, 2, step, width), lambda i: (0, 0, i, 0)),
        out_shape=jax.ShapeDtypeStruct((heads, 2, tokens, width), jnp.bfloat16),
        compiler_params=limit(16),
    )(first_position, freqs, q, k)


def weights_kernel(ratio_ref, qk_ref, out_ref, q_s, k_s, s_s, m_s, l_s):
    planes, _, tokens, width = qk_ref.shape
    blocks = planes * tokens // TILE
    step = pl.program_id(0)

    @pl.when(step == 0)
    def _():
        for z in range(planes):
            q_s[z * tokens : (z + 1) * tokens, :] = qk_ref[z, 0]
            k_s[z * tokens : (z + 1) * tokens, :] = qk_ref[z, 1]

    ratio = ratio_ref[0]

    def one_row(row, at):
        q = q_s[pl.ds(pl.multiple_of(row * TILE, TILE), TILE), :]
        lane = lax.broadcasted_iota(jnp.int32, (TILE, width), 1)
        zero = jnp.zeros_like(q)
        both = jnp.concatenate([jnp.where(lane < 64, q, zero), jnp.where(lane < 64, zero, q)], axis=0)

        def tile_scores(j):
            keys = k_s[pl.ds(pl.multiple_of(j * TILE, TILE), TILE), :]
            return lax.dot_general(
                both, keys, (((1,), (1,)), ((), ())), preferred_element_type=jnp.float32
            )

        r = lax.broadcasted_iota(jnp.int32, (2 * TILE, TILE), 0)
        c = lax.broadcasted_iota(jnp.int32, (2 * TILE, TILE), 1)
        s = jnp.where(r % TILE >= c, tile_scores(row), neg_large)
        s_s[row] = s
        m_s[...] = jnp.maximum(s[:, :128], s[:, 128:])

        @pl.loop(0, row)
        def _(j):
            s = tile_scores(j)
            s_s[j] = s
            m_s[...] = jnp.maximum(m_s[...], jnp.maximum(s[:, :128], s[:, 128:]))

        top = jnp.max(m_s[...], axis=-1, keepdims=True)
        m_s[...] = jnp.broadcast_to(top, m_s.shape)
        l_s[...] = jnp.zeros_like(l_s)

        @pl.loop(0, row + 1)
        def _(j):
            s = s_s[j]
            m = m_s[...]
            e0 = jnp.exp(s[:, :128] - m)
            e1 = jnp.exp(s[:, 128:] - m)
            l_s[...] += e0 + e1
            s_s[j] = jnp.concatenate([e0, e1], axis=1)

        total = jnp.sum(l_s[...], axis=-1, keepdims=True)
        a1 = 1.0 / total[:TILE]
        a2 = ratio / total[TILE:]
        l_s[...] = jnp.broadcast_to(jnp.concatenate([a1, a2], axis=0), l_s.shape)

        @pl.loop(0, row + 1)
        def _(j):
            b1 = l_s[:TILE, :]
            b2 = l_s[TILE:, :]
            e = s_s[j]
            w0 = e[:TILE, :128] * b1 - e[TILE:, :128] * b2
            w1 = e[:TILE, 128:] * b1 - e[TILE:, 128:] * b2
            lanes = pl.ds(pl.multiple_of((at + j) * TILE, TILE), TILE)
            out_ref[0, :, lanes] = jnp.concatenate([w0, w1], axis=1).astype(jnp.bfloat16)

    one_row(step, 0)
    one_row(blocks - 1 - step, step + 1)


def attention_weights(ratio, qk):
    planes, _, tokens, width = qk.shape
    blocks = planes * tokens // TILE
    return pl.pallas_call(
        weights_kernel,
        name="weights",
        grid=(blocks // 2,),
        in_specs=[
            SCALARS,
            pl.BlockSpec(qk.shape, lambda p: (0, 0, 0, 0)),
        ],
        out_specs=pl.BlockSpec((1, TILE, (blocks + 1) * TILE), lambda p: (p, 0, 0)),
        out_shape=pltpu.HBM((blocks // 2, TILE, (blocks + 1) * TILE), jnp.bfloat16),
        compiler_params=limit(60),
        scratch_shapes=[
            pltpu.VMEM((planes * tokens, width), jnp.bfloat16),
            pltpu.VMEM((planes * tokens, width), jnp.bfloat16),
            pltpu.VMEM((blocks, 2 * TILE, TILE), jnp.float32),
            pltpu.VMEM((2 * TILE, 128), jnp.float32),
            pltpu.VMEM((2 * TILE, 128), jnp.float32),
        ],
        cost_estimate=pl.CostEstimate(
            flops=8 * 10**9, bytes_accessed=14 * 10**6, transcendentals=10**7
        ),
    )(ratio, qk)


def mix_kernel(gain_ref, w_ref, v_ref, out_ref, w_s, sems):
    pairs = w_ref.shape[0]

    def fetch(p):
        return pltpu.make_async_copy(w_ref.at[p], w_s.at[p], sems.at[p])

    for p in range(pairs):
        fetch(p).start()
    for p in range(pairs):
        fetch(p).wait()
        split = (p + 1) * TILE
        for row, weights in ((p, w_s[p, :, :split]), (2 * pairs - 1 - p, w_s[p, :, split:])):
            mixed = jnp.dot(
                weights, v_ref[: (row + 1) * TILE, :], preferred_element_type=jnp.float32
            )
            scale = lax.rsqrt(jnp.mean(mixed * mixed, axis=-1, keepdims=True) + norm_eps)
            out_ref[row * TILE : (row + 1) * TILE, :] = (mixed * scale * gain_ref[...]).astype(
                jnp.bfloat16
            )


def mix_values(gain, w, v):
    planes, tokens, width = v.shape
    length = planes * tokens
    mixed = pl.pallas_call(
        mix_kernel,
        name="mix",
        in_specs=[WHOLE, IN_HBM, WHOLE],
        out_specs=WHOLE,
        out_shape=jax.ShapeDtypeStruct((length, width), jnp.bfloat16),
        scratch_shapes=[
            pltpu.VMEM(w.shape, jnp.bfloat16),
            pltpu.SemaphoreType.DMA((w.shape[0],)),
        ],
        compiler_params=limit(60),
    )(gain, w, in_vmem(v.reshape(length, width)))
    return mixed.reshape(planes, tokens, width)


def assemble_kernel(place_ref, *refs):
    pieces, (out_ref, sems) = refs[:8], refs[8:]
    place = place_ref[0]
    y, x, core = place // 8, place // 2 % 4, place % 2
    rows = pieces[0].shape[1]
    copies = []
    for s in range(4):
        for t in range(4):
            for other in range(2):
                at = (y + 4 - s) % 4 * 8 + (x + 4 - t) % 4 * 2 + (1 - core if other else core)
                copies.append(
                    pltpu.make_async_copy(
                        pieces[2 * s + other].at[t],
                        out_ref.at[pl.ds(pl.multiple_of(at * rows, rows), rows), :],
                        sems.at[s, t, other],
                    )
                )
    for copy in copies:
        copy.start()
    for copy in copies:
        copy.wait()


def assemble(place, pieces):
    _, rows, depth = pieces[0].shape
    return pl.pallas_call(
        assemble_kernel,
        name="assemble",
        in_specs=[SCALARS] + [IN_HBM] * len(pieces),
        out_specs=IN_HBM,
        out_shape=pltpu.HBM((32 * rows, depth), jnp.bfloat16),
        scratch_shapes=[pltpu.SemaphoreType.DMA((4, 4, 2))],
        compiler_params=limit(4),
    )(place, *pieces)


def project_kernel(a_ref, w_ref, out_ref, a_s, w_s, o_s, w_sems, o_sems):
    heads, tokens, width = a_ref.shape
    parts, step, _ = w_s.shape

    def fetch(c):
        return pltpu.make_async_copy(
            w_ref.at[c * step : (c + 1) * step, :], w_s.at[c], w_sems.at[c]
        )

    def put(c):
        return pltpu.make_async_copy(
            o_s.at[c], out_ref.at[:, c * step : (c + 1) * step], o_sems.at[c]
        )

    for c in range(parts):
        fetch(c).start()
    for h in range(heads):
        a_s[:, h * width : (h + 1) * width] = a_ref[h]
    for c in range(parts):
        fetch(c).wait()
        o_s[c] = lax.dot_general(
            a_s[...], w_s[c], (((1,), (1,)), ((), ())), preferred_element_type=jnp.float32
        ).astype(jnp.bfloat16)
        put(c).start()
    for c in range(parts):
        put(c).wait()


def project(attended, weight_rows):
    heads, tokens, width = attended.shape
    columns = weight_rows.shape[0]
    parts = 4
    return pl.pallas_call(
        project_kernel,
        name="project",
        in_specs=[WHOLE, IN_HBM],
        out_specs=IN_HBM,
        out_shape=jax.ShapeDtypeStruct((tokens, columns), jnp.bfloat16),
        scratch_shapes=[
            pltpu.VMEM((tokens, heads * width), jnp.bfloat16),
            pltpu.VMEM((parts, columns // parts, heads * width), jnp.bfloat16),
            pltpu.VMEM((parts, tokens, columns // parts), jnp.bfloat16),
            pltpu.SemaphoreType.DMA((parts,)),
            pltpu.SemaphoreType.DMA((parts,)),
        ],
        compiler_params=limit(60),
    )(in_vmem(attended), weight_rows)


def shifted(array, dy, dx, flip):
    def to(i):
        y, x, core = i // 8, i // 2 % 4, i % 2
        return (y + dy) % 4 * 8 + (x + dx) % 4 * 2 + (1 - core if flip else core)

    return lax.ppermute(array, "dp", [(i, to(i)) for i in range(32)])


def gather_same_core(rows):
    line = jnp.stack([rows] + [shifted(rows, 0, d, False) for d in (1, 2, 3)])
    return [line] + [shifted(line, d, 0, False) for d in (1, 2, 3)]


def with_other_core(planes):
    pieces = []
    for plane in planes:
        pieces += [plane, shifted(plane, 0, 0, True)]
    return pieces


def exchange(array):
    return lax.all_to_all(array, "sp", split_axis=0, concat_axis=0, tiled=True)


def on_device(queries, keys, values, mix_ratio, out_gain, out_weight):
    plane = lax.axis_index("sp")
    place = lax.axis_index("dp").astype(jnp.int32).reshape(1)
    tokens = queries.shape[1]
    first_position = (plane * tokens).astype(jnp.int32).reshape(1)
    ratio = lax.dynamic_slice_in_dim(mix_ratio, plane, 1, 0)
    grouped = turn_and_group(queries[0], keys[0], first_position)
    grouped, rows = lax.optimization_barrier((grouped, out_weight.T))
    qk = exchange(grouped)
    planes = gather_same_core(rows)
    by_head = jnp.swapaxes(values[0], 0, 1)
    by_head, qk, planes = lax.optimization_barrier((by_head, qk, planes))
    v = exchange(by_head)
    w = attention_weights(ratio, qk)
    attended = exchange(mix_values(out_gain[None, :], w, v))
    return project(attended, assemble(place, with_other_core(planes)))[None]


def solution(mesh):
    tokens = P("dp", "sp", None, None)
    return jax.shard_map(
        on_device,
        mesh=mesh,
        in_specs=(tokens, tokens, tokens, P(), P(), P(None, "dp")),
        out_specs=P("dp", "sp", None),
        check_vma=False,
    )
```
